32 devices in a mesh: fs: 8 (over z, y), tp: 4 (over x, core).
Axes of the slice: x: 2, y: 2, z: 4, core: 2. Of those that a mesh axis runs over, the one named last changes fastest.
Arguments:
- late_input: bfloat16 [2048, 2048], P(('fs', 'tp')), may hold values from -6 to 6
- early_input: bfloat16 [2048, 2048], P(('fs', 'tp')), may hold values from -6 to 6
- early_grad: bfloat16 [2048, 2048], P(('fs', 'tp')), may hold values from -6 to 6
- pre_gain: float32 [2048], replicated, may hold values from 0.1 to 1.9
- post_gain: float32 [2048], replicated, may hold values from 0.1 to 1.9
- gate_weight: bfloat16 [2048, 4096], P('fs', 'tp'), may hold values from -0.125 to 0.125
- up_weight: bfloat16 [2048, 4096], P('fs', 'tp'), may hold values from -0.125 to 0.125
- down_weight: bfloat16 [2048, 4096], P('fs', 'tp'), may hold values from -0.09375 to 0.09375
- gate_sum: float32 [2048, 4096], P('fs', 'tp'), may hold values from -1.8 to 1.8
- up_sum: float32 [2048, 4096], P('fs', 'tp'), may hold values from -1.8 to 1.8
- down_gradient_sum: float32 [2048, 4096], P('fs', 'tp'), may hold values from -1.8 to 1.8
Outputs:
- late_output: bfloat16 [2048, 2048], P(('fs', 'tp'))
- early_input_grad: bfloat16 [2048, 2048], P(('fs', 'tp'))
- gate_total: float32 [2048, 4096], P('fs', 'tp')
- up_total: float32 [2048, 4096], P('fs', 'tp')
- down_total: float32 [2048, 4096], P('fs', 'tp')
The draws below stay inside these ranges and needn't reach their ends.
All inputs are finite; a program needn't handle non-finite values.
Results may differ from the reference program's by a relative error of at most 0.013.
Values may be sent and summed in bfloat16 or wider, within the bound.
No kernel may reach another device: no remote copies, remote signals or barrier semaphores. Data moves between devices by JAX's collectives and lax.ppermute only.
A program may use at most 128 MiB of HBM per device.

```python
import math
import jax
import jax.numpy as jnp
from jax import lax

D = 2048
FF = 4096
ROWS = 2048
N_TP = 4


def with_spikes(array, rng, source, target, shards_of, factor):
    def block_of(position):
        return (jnp.arange(array.shape[position]) // (array.shape[position] // shards_of)).reshape((-1,) + (1,) * (array.ndim - 1 - position))

    one_side = jax.random.permutation(rng, shards_of)[block_of(target)]
    other_side = (block_of(target) + shards_of // 2) % shards_of
    return jnp.where((block_of(source) == one_side) | (block_of(source) == other_side), factor * array, array)


def shard_levels(own_key, shape, pieces, least, top_value):
    gain, own = 1.0, jax.random.fold_in(own_key, 6)
    for dim, shards_of in pieces:
        draws = jnp.exp(jax.random.uniform(jax.random.fold_in(own, dim), (shards_of,), jnp.float32, least / len(pieces), top_value / len(pieces)))
        gain = gain * jnp.repeat(draws, shape[dim] // shards_of).reshape([-1 if axis == dim else 1 for axis in range(len(shape))])
    return gain


def gaussian(rng, shape, scale, bound, split=(), held_as=jnp.bfloat16):
    loudness = shard_levels(rng, shape, split, -0.22, 0.18) if split else 1.0
    entries = jax.random.normal(rng, shape, jnp.float32) * scale * loudness
    return jnp.minimum(jnp.maximum(entries, -bound), bound).astype(held_as)


def noise_with(stream_key, shape, spread, limit, pieces, heavy, held_as=jnp.bfloat16):
    result = spread * jax.random.normal(stream_key, shape, jnp.float32)
    if pieces:
        result = result * shard_levels(stream_key, shape, pieces, -0.22, 0.18)
    return jnp.clip(with_spikes(result, jax.random.fold_in(stream_key, 3), *heavy), -limit, limit).astype(held_as)


def setup_inputs(seed: int = 0) -> dict:
    seeds = jax.random.split(jax.random.key(seed), 12)
    late_input = gaussian(seeds[0], (ROWS, D), 1.0, 6.0, ((0, 32),))
    early_input = gaussian(seeds[1], (ROWS, D), 1.0, 6.0, ((0, 32),))
    early_grad = noise_with(seeds[2], (ROWS, D), 1.0, 6.0, ((0, 32),), (0, 1, 32, 2.75))
    pre_gain = jnp.clip(1.0 + 0.18 * jax.random.normal(seeds[3], (D,), jnp.float32), 0.1, 1.9)
    post_gain = jnp.clip(1.0 + 0.18 * jax.random.normal(seeds[4], (D,), jnp.float32), 0.1, 1.9)
    gate_weight = gaussian(seeds[5], (D, FF), D ** -0.5, 0.125, ((0, 8), (1, 4)))
    up_weight = gaussian(seeds[6], (D, FF), D ** -0.5, 0.125, ((0, 8), (1, 4)))
    down_weight = gaussian(seeds[7], (D, FF), FF ** -0.5, 0.09375, ((0, 8), (1, 4)))
    gate_sum = gaussian(seeds[8], (D, FF), 0.3, 1.8, ((0, 8), (1, 4)), jnp.float32)
    up_sum = gaussian(seeds[9], (D, FF), 0.3, 1.8, ((0, 8), (1, 4)), jnp.float32)
    down_gradient_sum = gaussian(seeds[10], (D, FF), 0.3, 1.8, ((0, 8), (1, 4)), jnp.float32)
    return dict(late_input=late_input, early_input=early_input, early_grad=early_grad, pre_gain=pre_gain, post_gain=post_gain, gate_weight=gate_weight, up_weight=up_weight, down_weight=down_weight, gate_sum=gate_sum, up_sum=up_sum, down_gradient_sum=down_gradient_sum)


NORM_EPS = 1e-06

def contract_last(first_op, second_op):
    return lax.dot_general(first_op, second_op, (((1,), (1,)), ((), ())), preferred_element_type=jnp.float32)

def contract_first(first_op, second_op):
    return lax.dot_general(first_op, second_op, (((0,), (0,)), ((), ())), preferred_element_type=jnp.float32)

def inverse_rms(values):
    return lax.rsqrt(lax.optimization_barrier(jnp.mean(values * values, axis=-1, keepdims=True)) + NORM_EPS)

def rounded_blocks(term_of, row_count):
    running = jnp.zeros((row_count, D), jnp.float32)
    for block_index in range(N_TP):
        rounded = lax.optimization_barrier(term_of(block_index).astype(jnp.bfloat16))
        running = running + rounded.astype(jnp.float32)
    return running.astype(jnp.bfloat16)

def forward_rows(input_rows, pre_gain, gate_weight, up_weight, down_weight):
    values = input_rows.astype(jnp.float32)
    normed = (values * inverse_rms(values) * pre_gain).astype(jnp.bfloat16)
    gate_pre = jnp.dot(normed, gate_weight, preferred_element_type=jnp.float32)
    up_pre = jnp.dot(normed, up_weight, preferred_element_type=jnp.float32)
    hidden_state = (jax.nn.silu(gate_pre) * up_pre).astype(jnp.bfloat16)
    block_column_count = FF // N_TP

    def term_of(block_index):
        columns = slice(block_index * block_column_count, (block_index + 1) * block_column_count)
        return contract_last(hidden_state[:, columns], down_weight[:, columns])
    mixed = rounded_blocks(term_of, input_rows.shape[0])
    return (normed, gate_pre, up_pre, hidden_state, mixed)

def reference(late_input, early_input, early_grad, pre_gain, post_gain, gate_weight, up_weight, down_weight, gate_sum, up_sum, down_gradient_sum):
    late_mixed = forward_rows(late_input, pre_gain, gate_weight, up_weight, down_weight)[4]
    late_values = late_input.astype(jnp.float32)
    mixed_values = late_mixed.astype(jnp.float32)
    late_output = (late_values + 0.5 * mixed_values * inverse_rms(mixed_values) * post_gain).astype(jnp.bfloat16)
    normed, gate_pre, up_pre, hidden_state, mixed = forward_rows(early_input, pre_gain, gate_weight, up_weight, down_weight)
    early_mixed = mixed.astype(jnp.float32)
    inverse_norm = inverse_rms(early_mixed)
    weighted = 0.5 * early_grad.astype(jnp.float32) * post_gain
    mixed_cot = (inverse_norm * weighted - early_mixed * inverse_norm ** 3 * lax.optimization_barrier(jnp.mean(weighted * early_mixed, axis=-1, keepdims=True))).astype(jnp.bfloat16)
    hidden_cot = jnp.dot(mixed_cot, down_weight, preferred_element_type=jnp.float32)
    sigmoid_gate = jax.nn.sigmoid(gate_pre)
    gate_cot = (hidden_cot * up_pre * sigmoid_gate * (1.0 + gate_pre * (1.0 - sigmoid_gate))).astype(jnp.bfloat16)
    up_cot = (hidden_cot * gate_pre * sigmoid_gate).astype(jnp.bfloat16)
    block_column_count = FF // N_TP

    def back_term(block_index):
        columns = slice(block_index * block_column_count, (block_index + 1) * block_column_count)
        return contract_last(gate_cot[:, columns], gate_weight[:, columns]) + contract_last(up_cot[:, columns], up_weight[:, columns])
    normed_cot = rounded_blocks(back_term, early_input.shape[0]).astype(jnp.float32)
    early_values = early_input.astype(jnp.float32)
    early_inverse_norm = inverse_rms(early_values)
    weighted_in = normed_cot * pre_gain
    early_input_grad = (early_grad.astype(jnp.float32) + early_inverse_norm * weighted_in - early_values * early_inverse_norm ** 3 * lax.optimization_barrier(jnp.mean(weighted_in * early_values, axis=-1, keepdims=True))).astype(jnp.bfloat16)
    grad_scale = 1.0 / math.sqrt(ROWS)
    gate_total = gate_sum + grad_scale * contract_first(normed, gate_cot)
    up_total = up_sum + grad_scale * contract_first(normed, up_cot)
    down_total = down_gradient_sum + grad_scale * contract_first(mixed_cot, hidden_state)
    return (late_output, early_input_grad, gate_total, up_total, down_total)
```

```python
import math

import jax
import jax.numpy as jnp
from jax import lax
from jax.sharding import PartitionSpec as P

NORM_EPS = 1e-06
AXES = ("fs", "tp")


def contract_last(first_op, second_op):
    return lax.dot_general(
        first_op, second_op, (((1,), (1,)), ((), ())), preferred_element_type=jnp.float32
    )


def contract_first(first_op, second_op):
    return lax.dot_general(
        first_op, second_op, (((0,), (0,)), ((), ())), preferred_element_type=jnp.float32
    )


def matmul(first_op, second_op):
    return jnp.dot(first_op, second_op, preferred_element_type=jnp.float32)


def inverse_rms(values):
    return lax.rsqrt(jnp.mean(values * values, axis=-1, keepdims=True) + NORM_EPS)


def f32(values):
    return values.astype(jnp.float32)


def bf16(values):
    return values.astype(jnp.bfloat16)


class Grid:
    def __init__(self, mesh):
        devices = mesh.devices
        self.nz = len({d.coords[2] for d in devices.flat})
        self.ny = len({d.coords[1] for d in devices.flat})
        self.nx = len({d.coords[0] for d in devices.flat})
        self.nc = devices.shape[1] // self.nx

    def hop(self, value, dz=0, dy=0, dx=0, dc=0):
        nz, ny, nx, nc = self.nz, self.ny, self.nx, self.nc

        def flat(z, y, x, c):
            return ((z % nz * ny + y % ny) * nx + x % nx) * nc + c % nc

        pairs = [
            (flat(z, y, x, c), flat(z + dz, y + dy, x + dx, c + dc))
            for z in range(nz)
            for y in range(ny)
            for x in range(nx)
            for c in range(nc)
        ]
        return lax.ppermute(value, AXES, pairs)

    def position(self):
        fs = lax.axis_index("fs")
        return fs // self.ny, fs % self.ny

    def gather(self, value, axis, size):
        return [value] + [self.hop(value, **{axis: s}) for s in range(1, size)]

    def scatter(self, slots, axis):
        total = f32(slots[0])
        for s in range(1, len(slots)):
            total = total + f32(self.hop(slots[s], **{axis: -s}))
        return total


def build(grid):
    nz, ny, nx, nc = grid.nz, grid.ny, grid.nx, grid.nc

    def per_device(
        late_input,
        early_input,
        early_grad,
        pre_gain,
        post_gain,
        gate_weight,
        up_weight,
        down_weight,
        gate_sum,
        up_sum,
        down_gradient_sum,
    ):
        tok_rows, model_width = late_input.shape
        rows, columns = gate_weight.shape
        sub = columns // nz
        depth = nz * rows
        grad_scale = 1.0 / math.sqrt(tok_rows * nz * ny * nx * nc)
        z, y = grid.position()

        def to_slots(values):
            blocks = values.reshape(*values.shape[:-1], nz, ny, rows)
            parts = [
                lax.dynamic_index_in_dim(blocks, (y - s) % ny, blocks.ndim - 2, keepdims=False)
                for s in range(ny)
            ]
            return jnp.stack(parts, axis=-3).reshape(values.shape)

        def from_slots(values):
            blocks = values.reshape(*values.shape[:-1], ny, nz, rows)
            parts = [
                lax.dynamic_index_in_dim(blocks, (y - k) % ny, blocks.ndim - 3, keepdims=False)
                for k in range(ny)
            ]
            return jnp.stack(parts, axis=-2).reshape(values.shape)

        def exchange(weight):
            def part(k):
                return lax.dynamic_slice(weight, (0, k * sub), (rows, sub))

            out = jnp.zeros((depth, sub), weight.dtype)
            for s in range(nz):
                block = part((z + s) % nz)
                block = grid.hop(block, dz=s) if s else block
                out = lax.dynamic_update_slice(out, block, ((z - s) % nz * rows, 0))
            return out

        def gather_plane(block, x_first):
            r = block.shape[0]
            if x_first:
                line = jnp.stack(grid.gather(block, "dx", nx))
                both = jnp.stack(grid.gather(line, "dy", ny))
            else:
                line = jnp.stack(grid.gather(block, "dy", ny))
                both = jnp.stack(grid.gather(line, "dx", nx), axis=1)
            cores = grid.gather(both, "dc", nc)
            return [[[cores[c][j, i] for c in range(nc)] for i in range(nx)] for j in range(ny)]

        def assemble(pieces):
            return jnp.concatenate(
                [
                    jnp.concatenate([pieces[j][i][c] for i in range(nx) for c in range(nc)], axis=1)
                    for j in range(ny)
                ],
                axis=0,
            )

        early_rows = f32(to_slots(early_input))
        late_rows = f32(to_slots(late_input))
        grad_rows = f32(to_slots(early_grad))
        pre = to_slots(pre_gain)
        post = to_slots(post_gain)

        early_inverse = inverse_rms(early_rows)
        early_own = bf16(early_rows * early_inverse * pre)
        late_own = bf16(late_rows * inverse_rms(late_rows) * pre)

        gate_part = exchange(gate_weight)
        normed = jnp.concatenate(grid.gather(early_own, "dz", nz))
        up_part = exchange(up_weight)
        down_part = exchange(down_weight)
        gate_all = assemble(gather_plane(gate_part, True))
        up_all = assemble(gather_plane(up_part, False))
        half = depth // 2
        down_low = gather_plane(down_part[:half], True)
        down_high = gather_plane(down_part[half:], False)
        down_all = assemble(
            [
                [
                    [
                        jnp.concatenate([down_low[j][i][c], down_high[j][i][c]])
                        for c in range(nc)
                    ]
                    for i in range(nx)
                ]
                for j in range(ny)
            ]
        )
        late_normed = jnp.concatenate(grid.gather(late_own, "dz", nz))

        def hidden_of(tokens):
            gate_pre = matmul(tokens, gate_all)
            up_pre = matmul(tokens, up_all)
            return gate_pre, up_pre, bf16(jax.nn.silu(gate_pre) * up_pre)

        def token_sum(part):
            slots = [part[s * tok_rows : (s + 1) * tok_rows] for s in range(nz)]
            return f32(lax.optimization_barrier(bf16(grid.scatter(slots, "dz"))))

        gate_pre, up_pre, hidden = hidden_of(normed)
        mixed = token_sum(bf16(contract_last(hidden, down_all)))
        mixed_inverse = inverse_rms(mixed)
        weighted = 0.5 * grad_rows * post
        mixed_cot = bf16(
            mixed_inverse * weighted
            - mixed * mixed_inverse**3 * jnp.mean(weighted * mixed, axis=-1, keepdims=True)
        )
        cot_rows = jnp.concatenate(grid.gather(mixed_cot, "dz", nz))

        late_hidden = hidden_of(late_normed)[2]
        late_part = bf16(contract_last(late_hidden, down_all))

        hidden_cot = matmul(cot_rows, down_all)
        sigmoid_gate = jax.nn.sigmoid(gate_pre)
        gate_cot = bf16(hidden_cot * up_pre * sigmoid_gate * (1.0 + gate_pre * (1.0 - sigmoid_gate)))
        up_cot = bf16(hidden_cot * gate_pre * sigmoid_gate)

        def reduce_core(grad):
            blocks = bf16(grad).reshape(ny, depth, nx, nc, sub)
            return bf16(grid.scatter([blocks[:, :, :, c] for c in range(nc)], "dc"))

        def reduce_plane(blocks, x_first):
            if x_first:
                part = bf16(grid.scatter([blocks[:, :, i] for i in range(nx)], "dx"))
                return bf16(grid.scatter([part[j] for j in range(ny)], "dy"))
            part = bf16(grid.scatter([blocks[j] for j in range(ny)], "dy"))
            return bf16(grid.scatter([part[:, i] for i in range(nx)], "dx"))

        def exchange_back(part):
            blocks = part.reshape(nz, rows, sub)
            out = jnp.zeros((rows, columns), part.dtype)
            for s in range(nz):
                block = lax.dynamic_index_in_dim(blocks, (z + s) % nz, 0, keepdims=False)
                block = grid.hop(block, dz=s) if s else block
                out = lax.dynamic_update_slice(out, block, (0, (z - s) % nz * sub))
            return f32(out)

        down_blocks = reduce_core(contract_first(cot_rows, hidden))
        gate_blocks = reduce_core(contract_first(normed, gate_cot))
        up_blocks = reduce_core(contract_first(normed, up_cot))
        normed_cot_part = bf16(contract_last(gate_cot, gate_all) + contract_last(up_cot, up_all))
        down_grad = jnp.concatenate(
            [
                reduce_plane(down_blocks[:, :half], True),
                reduce_plane(down_blocks[:, half:], False),
            ]
        )
        gate_grad = reduce_plane(gate_blocks, True)
        up_grad = reduce_plane(up_blocks, False)

        normed_cot = token_sum(normed_cot_part)
        weighted_in = normed_cot * pre
        early_input_grad = bf16(
            grad_rows
            + early_inverse * weighted_in
            - early_rows
            * early_inverse**3
            * jnp.mean(weighted_in * early_rows, axis=-1, keepdims=True)
        )
        late_mixed = token_sum(late_part)
        late_output = bf16(late_rows + 0.5 * late_mixed * inverse_rms(late_mixed) * post)

        down_total = down_gradient_sum + grad_scale * exchange_back(down_grad)
        gate_total = gate_sum + grad_scale * exchange_back(gate_grad)
        up_total = up_sum + grad_scale * exchange_back(up_grad)
        return (
            from_slots(late_output),
            from_slots(early_input_grad),
            gate_total,
            up_total,
            down_total,
        )

    return per_device


def solution(mesh):
    tokens, weights = P(("fs", "tp"), None), P("fs", "tp")
    in_specs = (tokens,) * 3 + (P(),) * 2 + (weights,) * 6
    out_specs = (tokens,) * 2 + (weights,) * 3
    return jax.shard_map(
        build(Grid(mesh)), mesh=mesh, in_specs=in_specs, out_specs=out_specs, check_vma=False
    )
```

```python
import math

import jax
import jax.numpy as jnp
from jax import lax
from jax.experimental import pallas as pl
from jax.experimental.pallas import tpu as pltpu
from jax.sharding import PartitionSpec as P

NORM_EPS = 1e-06
AXES = ("fs", "tp")
VMEM_LIMIT = 12 * 2**20


def contract_last(first_op, second_op):
    return lax.dot_general(
        first_op, second_op, (((1,), (1,)), ((), ())), preferred_element_type=jnp.float32
    )


def contract_first(first_op, second_op):
    return lax.dot_general(
        first_op, second_op, (((0,), (0,)), ((), ())), preferred_element_type=jnp.float32
    )


def matmul(first_op, second_op):
    return jnp.dot(first_op, second_op, preferred_element_type=jnp.float32)


def inverse_rms(values):
    return lax.rsqrt(jnp.mean(values * values, axis=-1, keepdims=True) + NORM_EPS)


def f32(values):
    return values.astype(jnp.float32)


def bf16(values):
    return values.astype(jnp.bfloat16)


def after(value, *earlier):
    return lax.optimization_barrier((value, *earlier))[0]


class Grid:
    def __init__(self, mesh):
        devices = mesh.devices
        self.nz = len({d.coords[2] for d in devices.flat})
        self.ny = len({d.coords[1] for d in devices.flat})
        self.nx = len({d.coords[0] for d in devices.flat})
        self.nc = devices.shape[1] // self.nx
        self.mixed = self.nx == self.ny

    def hop(self, value, dz=0, dc=0, first=0, second=0):
        nz, ny, nx, nc = self.nz, self.ny, self.nx, self.nc

        def flat(z, y, x, c):
            return ((z % nz * ny + y % ny) * nx + x % nx) * nc + c % nc

        def target(z, y, x, c):
            dx, dy = (second, first) if self.mixed and c % 2 else (first, second)
            return flat(z + dz, y + dy, x + dx, c + dc)

        pairs = [
            (flat(z, y, x, c), target(z, y, x, c))
            for z in range(nz)
            for y in range(ny)
            for x in range(nx)
            for c in range(nc)
        ]
        return lax.ppermute(value, AXES, pairs)

    def position(self):
        fs = lax.axis_index("fs")
        return fs // self.ny, fs % self.ny

    def parities(self):
        core = lax.axis_index("tp") % self.nc
        turns = [(core - s) % self.nc % 2 if self.mixed else 0 * core for s in range(self.nc)]
        return jnp.stack(turns).astype(jnp.int32)

    def gather(self, value, axis, size):
        return [value] + [self.hop(value, **{axis: s}) for s in range(1, size)]

    def scatter(self, slots, axis):
        got = [slots[0]]
        return got + [self.hop(slots[s], **{axis: -s}) for s in range(1, len(slots))]


def sum_of(terms):
    total = terms[0]
    for term in terms[1:]:
        total = total + term
    return total


def add_all(terms):
    return bf16(sum_of([f32(term) for term in terms]))


class Kernels:
    def __init__(self, grid, tokens, depth, sub):
        self.nx, self.ny, self.nc = grid.nx, grid.ny, grid.nc
        self.tokens, self.depth, self.sub = tokens, depth, sub
        self.parities = grid.parities()
        self.flops = 2 * tokens * depth * sub * grid.nx * grid.ny * grid.nc

    def resident(self, body, inputs, outs, flops):
        bytes_moved = sum(a.size * a.dtype.itemsize for a in (*inputs, *outs))

        def with_pieces(turns, *refs):
            def block(ref, slot, x, y):
                odd = turns[slot]
                return ref[jnp.where(odd == 0, y, x), jnp.where(odd == 0, x, y)]

            body(block, *refs)

        return pl.pallas_call(
            with_pieces,
            in_specs=[pl.BlockSpec(memory_space=pltpu.SMEM)]
            + [pl.BlockSpec(memory_space=pltpu.VMEM)] * len(inputs),
            out_specs=[pl.BlockSpec(memory_space=pltpu.VMEM)] * len(outs),
            out_shape=outs,
            compiler_params=pltpu.CompilerParams(vmem_limit_bytes=VMEM_LIMIT),
            cost_estimate=pl.CostEstimate(flops=flops, transcendentals=0, bytes_accessed=bytes_moved),
        )(self.parities, *inputs)

    def slots(self, dtype):
        return jax.ShapeDtypeStruct((self.nx, self.nc, self.tokens, self.sub), dtype)

    def places(self):
        return [(i, c) for i in range(self.nx) for c in range(self.nc)]

    def columns(self, j):
        return slice(j * self.depth, (j + 1) * self.depth)

    def hidden(self, tokens, gate, up, keep):
        nc, ny = self.nc, self.ny

        def body(block, tok, *refs):
            gates, ups, outs = refs[:nc], refs[nc : 2 * nc], refs[2 * nc :]
            for i, c in self.places():
                g = sum_of([matmul(tok[:, self.columns(j)], block(gates[c], c, i, j)) for j in range(ny)])
                u = sum_of([matmul(tok[:, self.columns(j)], block(ups[c], c, i, j)) for j in range(ny)])
                outs[0][i, c] = bf16(g * jax.nn.sigmoid(g) * u)
                if keep:
                    outs[1][i, c] = g
                    outs[2][i, c] = u

        outs = [self.slots(jnp.bfloat16)] + ([self.slots(jnp.float32)] * 2 if keep else [])
        return self.resident(body, [tokens, *gate, *up], outs, 2 * self.flops)

    def to_rows(self, pairs):
        nc, n = self.nc, len(pairs)

        def body(block, *refs):
            rights, weights, out = refs[:n], refs[n:-1], refs[-1]
            for j in range(self.ny):
                terms = [
                    contract_last(rights[k][i, c], block(weights[k * nc + c], c, i, j))
                    for k in range(n)
                    for i, c in self.places()
                ]
                out[:, self.columns(j)] = bf16(sum_of(terms))

        inputs = [slots for slots, _ in pairs] + [piece for _, weight in pairs for piece in weight]
        outs = [jax.ShapeDtypeStruct((self.tokens, self.ny * self.depth), jnp.bfloat16)]
        return self.resident(body, inputs, outs, n * self.flops)[0]

    def cots(self, cot, gate_pre, up_pre, down):
        ny = self.ny

        def body(block, rows, gates, ups, *refs):
            downs, outs = refs[:-2], refs[-2:]
            for i, c in self.places():
                hidden_cot = sum_of(
                    [matmul(rows[:, self.columns(j)], block(downs[c], c, i, j)) for j in range(ny)]
                )
                g, u = gates[i, c], ups[i, c]
                s = jax.nn.sigmoid(g)
                outs[0][i, c] = bf16(hidden_cot * u * s * (1.0 + g * (1.0 - s)))
                outs[1][i, c] = bf16(hidden_cot * g * s)

        outs = [self.slots(jnp.bfloat16)] * 2
        return self.resident(body, [cot, gate_pre, up_pre, *down], outs, self.flops)

    def gradient(self, rows, slots, first):
        nc = self.nc

        def place(args):
            odd = args[1][0]
            return jnp.where(odd == 0, first, args[0]), jnp.where(odd == 0, args[0], first)

        def body(_, *refs):
            feats, rights, out = refs[:nc], refs[nc:-1], refs[-1]
            terms = [contract_first(f[...], right[0]) for f, right in zip(feats, rights)]
            out[0] = bf16(sum_of(terms))

        feature = pl.BlockSpec((self.tokens, self.depth), lambda *args: (0, place(args)[1]))
        unit = pl.BlockSpec((1, self.tokens, self.sub), lambda *args: (place(args)[0], 0, 0))
        shape = jax.ShapeDtypeStruct((self.ny, self.depth, self.sub), jnp.bfloat16)
        flops = self.flops // self.nx
        bytes_moved = sum(a.size * a.dtype.itemsize for a in (*rows, *slots)) + 2 * shape.size
        return pl.pallas_call(
            body,
            grid_spec=pltpu.PrefetchScalarGridSpec(
                num_scalar_prefetch=1,
                grid=(self.ny,),
                in_specs=[feature] * nc + [unit] * nc,
                out_specs=pl.BlockSpec((1, self.depth, self.sub), lambda i, _: (i, 0, 0)),
            ),
            out_shape=shape,
            compiler_params=pltpu.CompilerParams(
                dimension_semantics=("arbitrary",), vmem_limit_bytes=VMEM_LIMIT
            ),
            cost_estimate=pl.CostEstimate(flops=flops, transcendentals=0, bytes_accessed=bytes_moved),
        )(self.parities, *rows, *slots)


def build(grid):
    nz, ny, nx, nc = grid.nz, grid.ny, grid.nx, grid.nc

    def per_device(
        late_input,
        early_input,
        early_grad,
        pre_gain,
        post_gain,
        gate_weight,
        up_weight,
        down_weight,
        gate_sum,
        up_sum,
        down_gradient_sum,
    ):
        tok_rows, _ = late_input.shape
        rows, columns = gate_weight.shape
        sub = columns // nz
        depth = nz * rows
        grad_scale = 1.0 / math.sqrt(tok_rows * nz * ny * nx * nc)
        z, y = grid.position()

        def to_slots(values):
            blocks = values.reshape(*values.shape[:-1], nz, ny, rows)
            parts = [
                lax.dynamic_index_in_dim(blocks, (y - s) % ny, blocks.ndim - 2, keepdims=False)
                for s in range(ny)
            ]
            return jnp.stack(parts, axis=-3).reshape(values.shape)

        def from_slots(values):
            blocks = values.reshape(*values.shape[:-1], ny, nz, rows)
            parts = [
                lax.dynamic_index_in_dim(blocks, (y - k) % ny, blocks.ndim - 3, keepdims=False)
                for k in range(ny)
            ]
            return jnp.stack(parts, axis=-2).reshape(values.shape)

        def exchange(weight):
            def part(k):
                return lax.dynamic_slice(weight, (0, k * sub), (rows, sub))

            out = jnp.zeros((depth, sub), weight.dtype)
            for s in range(nz):
                block = part((z + s) % nz)
                block = grid.hop(block, dz=s) if s else block
                out = lax.dynamic_update_slice(out, block, ((z - s) % nz * rows, 0))
            return out

        def gather_plane(block):
            line = jnp.stack(grid.gather(block, "first", nx))
            both = jnp.stack(grid.gather(line, "second", ny))
            return grid.gather(both, "dc", nc)

        kernels = Kernels(grid, nz * tok_rows, depth, sub)

        early_rows = f32(to_slots(early_input))
        late_rows = f32(to_slots(late_input))
        grad_rows = f32(to_slots(early_grad))
        pre = to_slots(pre_gain)
        post = to_slots(post_gain)

        early_inverse = inverse_rms(early_rows)
        early_own = bf16(early_rows * early_inverse * pre)
        late_own = bf16(late_rows * inverse_rms(late_rows) * pre)

        gate_part = exchange(gate_weight)
        up_part = exchange(after(up_weight, gate_part, early_own, late_own))
        down_part = exchange(after(down_weight, up_part, grad_rows))

        def gather_tokens(own):
            return jnp.concatenate(grid.gather(own, "dz", nz))

        normed = gather_tokens(after(early_own, down_part))
        late_got_rows = grid.gather(after(late_own, normed), "dz", nz)
        gate = gather_plane(gate_part)
        up = gather_plane(up_part)
        down = gather_plane(down_part)

        def send_tokens(part):
            slots = [part[s * tok_rows : (s + 1) * tok_rows] for s in range(nz)]
            return grid.scatter(slots, "dz")

        def token_sum(terms):
            return f32(lax.optimization_barrier(add_all(terms)))

        hidden, gate_pre, up_pre = kernels.hidden(normed, gate, up, True)
        part = kernels.to_rows([(hidden, down)])
        late_normed = jnp.concatenate([after(piece, part) for piece in late_got_rows])
        mixed = token_sum(send_tokens(part))
        mixed_inverse = inverse_rms(mixed)
        weighted = 0.5 * grad_rows * post
        mixed_cot = bf16(
            mixed_inverse * weighted
            - mixed * mixed_inverse**3 * jnp.mean(weighted * mixed, axis=-1, keepdims=True)
        )
        cot_rows = gather_tokens(mixed_cot)

        late_hidden = kernels.hidden(late_normed, gate, up, False)[0]
        late_part = kernels.to_rows([(late_hidden, down)])
        cot_rows = after(cot_rows, late_part)

        def columns_here(slots):
            return grid.scatter([slots[:, c] for c in range(nc)], "dc")

        def gradients(rows, slots):
            result = [None] * nx
            for k in (*range(1, nx), 0):
                result[k] = kernels.gradient(rows, slots, k)
            return result

        def lines_of(sums):
            got = grid.scatter(sums, "first")
            lines = [None] * ny
            for k in (*range(1, ny), 0):
                lines[k] = add_all([term[k] for term in got])
            return lines

        def send_back(part):
            blocks = part.reshape(nz, rows, sub)
            sent = [
                lax.dynamic_index_in_dim(blocks, (z + s) % nz, 0, keepdims=False)
                for s in range(nz)
            ]
            return [grid.hop(sent[s], dz=s) if s else sent[s] for s in range(nz)]

        def columns_of(blocks):
            out = jnp.zeros((rows, columns), blocks[0].dtype)
            for s in range(nz):
                out = lax.dynamic_update_slice(out, blocks[s], (0, (z - s) % nz * sub))
            return f32(out)

        both_normed = grid.gather(normed, "dc", nc)
        both_hidden = columns_here(hidden)
        both_cot = grid.gather(cot_rows, "dc", nc)
        late_got = send_tokens(after(late_part, cot_rows))
        gate_cot, up_cot = kernels.cots(cot_rows, gate_pre, up_pre, down)
        both_gate_cot = columns_here(gate_cot)
        both_up_cot = columns_here(up_cot)
        down_sums = gradients(both_cot, both_hidden)
        gate_sums = gradients(both_normed, both_gate_cot)
        up_sums = gradients(both_normed, both_up_cot)
        normed_cot_part = kernels.to_rows([(gate_cot, gate), (up_cot, up)])
        cot_got = send_tokens(normed_cot_part)
        down_lines = lines_of(down_sums)
        gate_lines = lines_of(gate_sums)
        up_lines = lines_of(up_sums)
        down_got = grid.scatter(down_lines, "second")
        gate_got = grid.scatter(gate_lines, "second")
        up_got = grid.scatter(up_lines, "second")
        down_grad = add_all([after(term, up_lines[-1]) for term in down_got])
        down_back = send_back(down_grad)
        gate_back = send_back(add_all(gate_got))
        up_grad = add_all(up_got)
        up_back = send_back(up_grad)
        late_mixed = token_sum(late_got)
        late_output = bf16(late_rows + 0.5 * late_mixed * inverse_rms(late_mixed) * post)
        normed_cot = token_sum(cot_got)
        weighted_in = normed_cot * pre
        early_input_grad = bf16(
            grad_rows
            + early_inverse * weighted_in
            - early_rows
            * early_inverse**3
            * jnp.mean(weighted_in * early_rows, axis=-1, keepdims=True)
        )
        late_output = from_slots(late_output)
        early_input_grad = from_slots(early_input_grad)
        down_total = down_gradient_sum + grad_scale * columns_of(down_back)
        gate_total = gate_sum + grad_scale * columns_of(gate_back)
        up_total = up_sum + grad_scale * columns_of(up_back)
        return late_output, early_input_grad, gate_total, up_total, down_total

    return per_device


def solution(mesh):
    grid = Grid(mesh)
    tokens, weights = P(("fs", "tp"), None), P("fs", "tp")
    in_specs = (tokens,) * 3 + (P(),) * 2 + (weights,) * 6
    out_specs = (tokens,) * 2 + (weights,) * 3
    per_device = build(grid)

    return jax.shard_map(per_device, mesh=mesh, in_specs=in_specs, out_specs=out_specs, check_vma=False)
```
